32 devices in a mesh: sp: 8 (over z, y), tp: 4 (over x, core).
Axes of the slice: x: 2, y: 2, z: 4, core: 2. Of those that a mesh axis runs over, the one named last changes fastest.
Arguments:
- residual: bfloat16 [2048, 2048], P(('sp', 'tp')), may hold values from -6 to 6
- output_gate_projected: bfloat16 [2048, 4096], P('sp', 'tp'), may hold values from -6 to 6
- value_projected_input: bfloat16 [2048, 4096], P('sp', 'tp'), may hold values from -6 to 6
- state_projected_input: bfloat16 [2048, 2048], P('sp', 'tp'), may hold values from -6 to 6
- readout_projected_input: bfloat16 [2048, 2048], P('sp', 'tp'), may hold values from -6 to 6
- step_preactivation: float32 [2048, 64], P('sp', 'tp'), may hold values from -5 to 5
- position_decay_extra: float32 [2048, 64], P('sp', 'tp')
- value_conv_kernel: bfloat16 [4, 4096], P(None, 'tp'), may hold values from -0.29882812 to 0.29882812
- state_conv_kernel: bfloat16 [4, 2048], P(None, 'tp'), may hold values from -0.8984375 to 0.8984375
- readout_conv_kernel: bfloat16 [4, 2048], P(None, 'tp'), may hold values from -0.8984375 to 0.8984375
- head_log_decay_rates: float32 [64], P('tp')
- head_direct_weight: float32 [64], P('tp'), may hold values from 0.5 to 4
- head_norm_gain: float32 [4096], P('tp'), may hold values from 0.1 to 1.9
- mixer_output_weight: bfloat16 [4096, 2048], P('tp'), may hold values from -0.09375 to 0.09375
- expert_norm_gain: float32 [2048], replicated, may hold values from 0.1 to 1.9
- routed_expert_index: int32 [2048, 4], P(('sp', 'tp')), may hold values from 0 to 7, all different within a row; in each aligned block of 64 rows (0 to 63, 64 to 127, ...) at most 64 rows name the same one
- routed_expert_weight: float32 [2048, 4], P(('sp', 'tp')), may hold values from 0.2 to 1
- routed_gate_weight: bfloat16 [8, 2048, 256], P('sp'), may hold values from -0.125 to 0.125
- routed_up_weight: bfloat16 [8, 2048, 256], P('sp'), may hold values from -0.125 to 0.125
- routed_down_weight: bfloat16 [8, 256, 2048], P('sp'), may hold values from -0.375 to 0.375
- common_gate_weight: bfloat16 [2048, 512], P(None, 'tp'), may hold values from -0.125 to 0.125
- common_up_weight: bfloat16 [2048, 512], P(None, 'tp'), may hold values from -0.125 to 0.125
- common_down_weight: bfloat16 [2048, 512], P(None, 'tp'), may hold values from -0.25 to 0.25
Outputs:
- layer_out: bfloat16 [2048, 2048], P(('sp', 'tp'))
The draws below stay inside these ranges and needn't reach their ends.
Inputs may be any that keep to these rules, and one draw needn't show every extreme that they name: `routed_expert_index`: among the 64 rows of one device, no expert is named by more than 64 rows.
All inputs are finite; a program needn't handle non-finite values.
Results may differ from the reference program's by a relative error of at most 0.02.
Values may be sent and summed in bfloat16 or wider, within the bound.
A program may use at most 128 MiB of HBM per device.

```python
import math
import jax
import jax.numpy as jnp
import numpy as np
from jax import lax

D = 2048
HEAD_DIM = 64
HEADS = 64
HEAD_GROUPS = 16
STATE = 128
CONV = 4
BLOCK_POSITIONS = 128
FE = 256
FS = 512
TOPK = 4
TOK_DEV = 256
INNER = 4096
SEQ = 2048
ROWS = 64
EXPERTS = 8
CAP = 64
N_TP = 4


def draw_step_preactivation(key, part):
    base_key, shift_key = jax.random.split(jax.random.fold_in(key, 11))
    block_list = SEQ // TOK_DEV
    jitter = jnp.clip(jax.random.normal(base_key, (SEQ, HEADS), jnp.float32), -4.0, 4.0)
    offsets = jax.random.uniform(shift_key, (block_list, 1, HEADS), jnp.float32, -1.0, 1.0)
    return (jitter.reshape(block_list, TOK_DEV, HEADS) + offsets).reshape(SEQ, HEADS)


def draw_head_log_decay_rates(key, part):
    pick_key, fast_key, slow_key = jax.random.split(jax.random.fold_in(key, 23), 3)
    ranking = jax.random.permutation(pick_key, HEADS)
    fast = ranking < HEADS // 2
    fast_rate = jax.random.uniform(fast_key, (HEADS,), jnp.float32, math.log(2.0 / BLOCK_POSITIONS), math.log(6.0 / BLOCK_POSITIONS))
    slow_rate = jax.random.uniform(slow_key, (HEADS,), jnp.float32, math.log(0.1 / SEQ), math.log(0.6 / SEQ))
    return jnp.where(fast, fast_rate, slow_rate)


def draw_position_decay_extra(key, part):
    place_key, depth_key = jax.random.split(jax.random.fold_in(key, 37))
    places = jax.random.randint(place_key, (3,), 0, SEQ)
    depths = jax.random.uniform(depth_key, (3, HEADS), jnp.float32, math.log(0.6), math.log(0.8))
    return jnp.zeros((SEQ, HEADS), jnp.float32).at[places].add(depths)


def steps_of(rng, dims, pieces, least, high):
    def one(position, parts):
        heights = jax.random.uniform(jax.random.fold_in(jax.random.fold_in(rng, 6), position), (parts,), jnp.float32, least / len(pieces), high / len(pieces))
        return jnp.repeat(jnp.exp(heights), dims[position] // parts).reshape((-1,) + (1,) * (len(dims) - position - 1))

    loudness = one(*pieces[0])
    for cut in pieces[1:]:
        loudness = loudness * one(*cut)
    return loudness


def assign_block(own_key, own, number, rows, count, top, bound, slope):
    sequence = jax.random.permutation(own_key, count)
    packed, common = load_shares(count, rows * top, bound, slope, True), load_shares(count, rows * top, bound, slope, False)
    places = jnp.arange(count)

    def named(tallies, turn):
        used = int((tallies > 0).sum())
        fixed = max(1, used // 4)
        moved = fixed + (places - fixed + turn * (used - fixed)) % max(1, count - fixed)
        return jnp.zeros((count,), jnp.int32).at[sequence[jnp.where(places < fixed, places, moved)]].set(jnp.asarray(tallies, jnp.int32))

    tallies = jnp.where(number % 4 == 0, named(packed, number // 4), named(common, number - number // 4 - 1))
    mixed = jax.random.permutation(jax.random.fold_in(own, 3), count)
    source_of, sink = mixed[0:count // 2 * 2:2], mixed[1:count // 2 * 2:2]
    slack = jnp.minimum(tallies[source_of] - 1, bound - tallies[sink]) // 2
    slack = jnp.where((source_of == sequence[0]) | (sink == sequence[0]) | (tallies[sink] == 0), 0, jnp.maximum(slack, 0))
    moved = jax.random.randint(jax.random.fold_in(own, 4), (count // 2,), 0, 1 << 20) % (slack + 1)
    tallies = tallies.at[source_of].add(-moved).at[sink].add(moved)
    members = jnp.searchsorted(jnp.cumsum(tallies), jnp.arange(rows * top), side="right").astype(jnp.int32)
    table = members.reshape(top, rows).T
    table = table[jax.random.permutation(jax.random.fold_in(own, 1), rows)]
    turn = jax.random.randint(jax.random.fold_in(own, 2), (rows, 1), 0, top)
    return jnp.take_along_axis(table, (jnp.arange(top)[None, :] + turn) % top, axis=1)


def load_shares(number_of, total, reach, lean, full):
    portions = [(1 << 20) // math.isqrt(grade ** lean) + 1 for grade in range(1, number_of + 1)]
    largest = reach if full else min(reach, max(-(-total // number_of), total * portions[0] // sum(portions)))
    least = 1 if total - largest >= number_of - 1 else 0
    holding, surplus = [largest] + [least] * (number_of - 1), total - largest - least * (number_of - 1)
    while surplus > 0:
        candidates = [i for i in range(1, number_of) if holding[i] < largest] or [i for i in range(1, number_of) if holding[i] < reach]
        mass, remaining = sum([portions[i] for i in candidates]), surplus
        for i in candidates:
            more = min(reach - holding[i], max(1, remaining * portions[i] // mass), surplus)
            holding[i] = holding[i] + more
            surplus = surplus - more
    return np.array(holding)


def scatter_about(rng, dims, deviation, most, pieces=(), held_as=jnp.bfloat16):
    values = deviation * jax.random.normal(rng, dims, jnp.float32)
    if pieces:
        values = values * steps_of(rng, dims, pieces, -0.22, 0.18)
    return jnp.clip(values, -most, most).astype(held_as)


def setup_inputs(seed: int = 0) -> dict:
    arg_keys = jax.random.split(jax.random.key(seed), 24)
    residual = scatter_about(arg_keys[0], (SEQ, D), 1.0, 6.0, ((0, 32),))
    output_gate_projected = scatter_about(arg_keys[1], (SEQ, INNER), 1.0, 6.0, ((0, 8), (1, 4)))
    value_projected_input = scatter_about(arg_keys[2], (SEQ, INNER), 1.0, 6.0, ((0, 8), (1, 4)))
    state_projected_input = scatter_about(arg_keys[3], (SEQ, HEAD_GROUPS * STATE), 1.0, 6.0, ((0, 8), (1, 4)))
    readout_projected_input = scatter_about(arg_keys[4], (SEQ, HEAD_GROUPS * STATE), 1.0, 6.0, ((0, 8), (1, 4)))
    step_preactivation = draw_step_preactivation(jax.random.fold_in(arg_keys[23], 71), 0)
    position_decay_extra = draw_position_decay_extra(jax.random.fold_in(arg_keys[23], 71), 0)
    value_conv_kernel = scatter_about(arg_keys[7], (CONV, INNER), 0.05, 0.29882812, ((1, 4),))
    state_conv_kernel = scatter_about(arg_keys[8], (CONV, HEAD_GROUPS * STATE), 0.15, 0.8984375, ((1, 4),))
    readout_conv_kernel = scatter_about(arg_keys[9], (CONV, HEAD_GROUPS * STATE), 0.15, 0.8984375, ((1, 4),))
    head_log_decay_rates = draw_head_log_decay_rates(jax.random.fold_in(arg_keys[23], 71), 0)
    head_direct_weight = jnp.clip(jnp.exp(math.log(4.0) - 2.0794415 * jax.random.uniform(arg_keys[11], (HEADS,), jnp.float32) ** steps_of(arg_keys[11], (HEADS,), ((0, 4),), -0.2, 0.2)), 0.5, 4.0)
    head_norm_gain = jnp.clip(1.0 + 0.18 * jax.random.normal(arg_keys[12], (INNER,), jnp.float32), 0.1, 1.9)
    mixer_output_weight = scatter_about(arg_keys[13], (INNER, D), INNER ** -0.5, 0.09375, ((0, 4),))
    expert_norm_gain = jnp.clip(1.0 + 0.18 * jax.random.normal(arg_keys[14], (D,), jnp.float32), 0.1, 1.9)
    routed_expert_index_keys = jax.random.split(jax.random.fold_in(arg_keys[15], 1), SEQ // ROWS)
    routed_expert_index_turns = jax.random.permutation(jax.random.fold_in(arg_keys[15], 3), SEQ // ROWS)
    routed_expert_index = jax.vmap(lambda own, number: assign_block(jax.random.fold_in(arg_keys[15], 2), own, number, ROWS, EXPERTS, TOPK, CAP, 2))(routed_expert_index_keys, routed_expert_index_turns).reshape((SEQ, TOPK))
    routed_expert_weight = jnp.clip(0.2 + 0.8 * jax.random.uniform(arg_keys[16], (SEQ, TOPK), jnp.float32) ** steps_of(arg_keys[16], (SEQ, TOPK), ((0, 32),), -0.2, 0.2), 0.2, 1.0)
    routed_gate_weight = scatter_about(arg_keys[17], (EXPERTS, D, FE), D ** -0.5, 0.125, ((0, 8),))
    routed_up_weight = scatter_about(arg_keys[18], (EXPERTS, D, FE), D ** -0.5, 0.125, ((0, 8),))
    routed_down_weight = scatter_about(arg_keys[19], (EXPERTS, FE, D), FE ** -0.5, 0.375, ((0, 8),))
    common_gate_weight = scatter_about(arg_keys[20], (D, FS), D ** -0.5, 0.125, ((1, 4),))
    common_up_weight = scatter_about(arg_keys[21], (D, FS), D ** -0.5, 0.125, ((1, 4),))
    common_down_weight = scatter_about(arg_keys[22], (D, FS), FS ** -0.5, 0.25, ((1, 4),))
    return dict(residual=residual, output_gate_projected=output_gate_projected, value_projected_input=value_projected_input, state_projected_input=state_projected_input, readout_projected_input=readout_projected_input, step_preactivation=step_preactivation, position_decay_extra=position_decay_extra, value_conv_kernel=value_conv_kernel, state_conv_kernel=state_conv_kernel, readout_conv_kernel=readout_conv_kernel, head_log_decay_rates=head_log_decay_rates, head_direct_weight=head_direct_weight, head_norm_gain=head_norm_gain, mixer_output_weight=mixer_output_weight, expert_norm_gain=expert_norm_gain, routed_expert_index=routed_expert_index, routed_expert_weight=routed_expert_weight, routed_gate_weight=routed_gate_weight, routed_up_weight=routed_up_weight, routed_down_weight=routed_down_weight, common_gate_weight=common_gate_weight, common_up_weight=common_up_weight, common_down_weight=common_down_weight)


EPSILON = 1e-06
HIGHEST_PRECISION = lax.Precision.HIGHEST

def short_conv(inputs, weights):
    length = inputs.shape[0]
    padded = jnp.pad(inputs.astype(jnp.float32), ((CONV - 1, 0), (0, 0)))
    totals = jnp.zeros((length, inputs.shape[1]), jnp.float32)
    for tap_index in range(CONV):
        totals = totals + padded[tap_index:tap_index + length] * weights[tap_index].astype(jnp.float32)
    return jax.nn.silu(totals)

def swiglu_rows(rows, gate_weight, up_weight, down_weight):
    gate_part = jnp.dot(rows, gate_weight, preferred_element_type=jnp.float32)
    lifted = jnp.dot(rows, up_weight, preferred_element_type=jnp.float32)
    hidden = (jax.nn.silu(gate_part) * lifted).astype(jnp.bfloat16)
    return jnp.dot(hidden, down_weight, preferred_element_type=jnp.float32)

def reference(residual, output_gate_projected, value_projected_input, state_projected_input, readout_projected_input, step_preactivation, position_decay_extra, value_conv_kernel, state_conv_kernel, readout_conv_kernel, head_log_decay_rates, head_direct_weight, head_norm_gain, mixer_output_weight, expert_norm_gain, routed_expert_index, routed_expert_weight, routed_gate_weight, routed_up_weight, routed_down_weight, common_gate_weight, common_up_weight, common_down_weight):
    heads_per_group = HEADS // HEAD_GROUPS
    block_list = SEQ // BLOCK_POSITIONS
    values = short_conv(value_projected_input, value_conv_kernel).reshape(block_list, BLOCK_POSITIONS, HEAD_GROUPS, heads_per_group, HEAD_DIM)
    state_in = short_conv(state_projected_input, state_conv_kernel).reshape(block_list, BLOCK_POSITIONS, HEAD_GROUPS, STATE)
    readout = short_conv(readout_projected_input, readout_conv_kernel).reshape(block_list, BLOCK_POSITIONS, HEAD_GROUPS, STATE)
    head_step_lengths = jax.nn.softplus(step_preactivation)
    decay_logarithm = (head_step_lengths * (-jnp.exp(head_log_decay_rates))[None, :] + position_decay_extra).reshape(block_list, BLOCK_POSITIONS, HEAD_GROUPS, heads_per_group)
    head_step_lengths = head_step_lengths.reshape(block_list, BLOCK_POSITIONS, HEAD_GROUPS, heads_per_group)
    gates = output_gate_projected.reshape(block_list, BLOCK_POSITIONS, HEADS, HEAD_DIM)
    streams = residual.reshape(block_list, BLOCK_POSITIONS, D)
    skips = head_direct_weight.reshape(HEAD_GROUPS, heads_per_group)
    gains = head_norm_gain.reshape(HEADS, HEAD_DIM)
    out_parts = mixer_output_weight.astype(jnp.float32).reshape(N_TP, INNER // N_TP, D)
    causal = jnp.arange(BLOCK_POSITIONS)[:, None] >= jnp.arange(BLOCK_POSITIONS)[None, :]

    def block_step(carried, block_inputs):
        value_blk, input_blk, readout_blk, decay_blk, sizes_blk, gate_blk, stream_blk = block_inputs
        cumulative = jnp.cumsum(decay_blk, axis=0)
        weighted_output = value_blk * sizes_blk[..., None]
        by_head = jnp.transpose(cumulative, (1, 2, 0))
        span_logs = by_head[:, :, :, None] - by_head[:, :, None, :]
        decay_factors = jnp.exp(jnp.where(causal, span_logs, -jnp.inf))
        attention_scores = jnp.einsum('tgn,sgn->gts', readout_blk, input_blk, precision=HIGHEST_PRECISION)
        within_block_output = jnp.einsum('wkij,jwke->iwke', attention_scores[:, None] * decay_factors, weighted_output, precision=HIGHEST_PRECISION)
        carried_out = jnp.einsum('tgn,grpn->tgrp', readout_blk, carried, precision=HIGHEST_PRECISION) * jnp.exp(cumulative)[..., None]
        mixed_heads = within_block_output + carried_out + skips[None, :, :, None] * value_blk
        to_end = jnp.exp(cumulative[-1:] - cumulative)
        fresh_state = jnp.einsum('sgn,sgrp->grpn', input_blk, weighted_output * to_end[..., None], precision=HIGHEST_PRECISION)
        carried = jnp.exp(cumulative[-1])[..., None, None] * carried + fresh_state
        mixed_heads = mixed_heads.reshape(BLOCK_POSITIONS, HEADS, HEAD_DIM) * jax.nn.silu(gate_blk.astype(jnp.float32))
        normed = mixed_heads * lax.rsqrt(lax.optimization_barrier(jnp.mean(mixed_heads * mixed_heads, axis=-1, keepdims=True)) + EPSILON) * gains
        heads_out = lax.optimization_barrier(normed.astype(jnp.bfloat16)).astype(jnp.float32)
        heads_out = heads_out.reshape(BLOCK_POSITIONS, N_TP, INNER // N_TP)
        partials = jnp.einsum('tqi,qid->qtd', heads_out, out_parts).astype(jnp.bfloat16)
        partials = lax.optimization_barrier(partials).astype(jnp.float32)
        stream = stream_blk.astype(jnp.float32) + lax.optimization_barrier(jnp.sum(partials, axis=0))
        return (carried, stream.astype(jnp.bfloat16))
    start_state = jnp.zeros((HEAD_GROUPS, heads_per_group, HEAD_DIM, STATE), jnp.float32)
    _, stream = lax.scan(block_step, start_state, (values, state_in, readout, decay_logarithm, head_step_lengths, gates, streams))
    stream = stream.reshape(SEQ, D).astype(jnp.float32)
    normed_rows = (stream * lax.rsqrt(lax.optimization_barrier(jnp.mean(stream * stream, axis=-1, keepdims=True)) + EPSILON) * expert_norm_gain).astype(jnp.bfloat16)
    shared = swiglu_rows(normed_rows, common_gate_weight, common_up_weight, common_down_weight.T)
    group_rows = 128
    tokens = SEQ
    assignments = tokens * TOPK
    flat_ids = routed_expert_index.reshape(-1).astype(jnp.int32)
    sort_order = jnp.argsort(flat_ids).astype(jnp.int32)
    sorted_ids = flat_ids[sort_order]
    counts = lax.optimization_barrier(jnp.sum((flat_ids[:, None] == jnp.arange(EXPERTS, dtype=jnp.int32)[None, :]).astype(jnp.int32), axis=0)).astype(jnp.int32)
    padded = ((counts + group_rows - 1) // group_rows * group_rows).astype(jnp.int32)
    starts = (jnp.cumsum(counts) - counts).astype(jnp.int32)
    pad_end = jnp.cumsum(padded).astype(jnp.int32)
    pad_start = (pad_end - padded).astype(jnp.int32)
    destination = (pad_start[sorted_ids] + jnp.arange(assignments, dtype=jnp.int32) - starts[sorted_ids]).astype(jnp.int32)
    nblocks = -(-assignments // group_rows) + EXPERTS
    rows_total = nblocks * group_rows
    row_token = jnp.full((rows_total,), tokens, jnp.int32).at[destination].set((sort_order // TOPK).astype(jnp.int32))
    row_weight = jnp.zeros((rows_total,), jnp.float32).at[destination].set(routed_expert_weight.reshape(-1)[sort_order])
    block_expert = jnp.minimum(jnp.searchsorted(pad_end, jnp.arange(nblocks, dtype=jnp.int32) * group_rows, side='right'), EXPERTS - 1).astype(jnp.int32)
    padded_rows = jnp.concatenate([normed_rows, jnp.zeros((1, D), jnp.bfloat16)], axis=0)

    def expert_block(block_args):
        token_ids, expert_id = block_args
        chosen = padded_rows[token_ids]
        return swiglu_rows(chosen, routed_gate_weight[expert_id], routed_up_weight[expert_id], routed_down_weight[expert_id]).astype(jnp.bfloat16)
    outputs = lax.map(expert_block, (row_token.reshape(nblocks, group_rows), block_expert))
    contrib = outputs.reshape(rows_total, D).astype(jnp.float32) * row_weight[:, None]
    routed = jnp.zeros((tokens + 1, D), jnp.float32).at[row_token].add(contrib)[:tokens]
    return (stream + shared + routed).astype(jnp.bfloat16)
```

```python
import functools

import jax
import jax.numpy as jnp
from jax import lax
from jax.experimental import pallas as pl
from jax.experimental.pallas import tpu as pltpu
from jax.sharding import PartitionSpec as P

HEAD_DIM = 64
STATE = 128
CONV = 4
EPSILON = 1e-06
EXACT = lax.Precision.HIGHEST
F32 = jnp.float32
BF16 = jnp.bfloat16


def head_lanes(heads):
    lane_head = lax.broadcasted_iota(jnp.int32, (heads, heads * HEAD_DIM), 1) // HEAD_DIM
    return (lane_head == lax.broadcasted_iota(jnp.int32, lane_head.shape, 0)).astype(F32)


def expand(per_head, lanes):
    return jnp.dot(per_head, lanes, precision=EXACT, preferred_element_type=F32)


def silu(value):
    return value / (1.0 + jnp.exp(-value))


def local_kernel(
    v_ref, b_ref, c_ref, rim_ref, pre_ref, extra_ref, rates_ref, skip_ref, vk_ref, bk_ref, ck_ref,
    state_ref, y_ref, readout_ref, cum_ref, v_ext, b_ext, c_ext,
):
    length, heads = pre_ref.shape
    groups = b_ref.shape[1] // STATE
    per_group = heads // groups
    pad = rim_ref.shape[0]

    def conv(x_ref, first, k_ref, ext):
        width = x_ref.shape[1]
        ext[:pad] = rim_ref[:, first : first + width].astype(F32)
        ext[pad:] = x_ref[...].astype(F32)
        total = jnp.zeros((length, width), F32)
        for tap in range(CONV):
            start = pad - CONV + 1 + tap
            total += ext[start : start + length] * k_ref[tap : tap + 1].astype(F32)
        return silu(total)

    step = pre_ref[...]
    step = jnp.maximum(step, 0.0) + jnp.log1p(jnp.exp(-jnp.abs(step)))
    log_decay = -jnp.exp(rates_ref[...]) * step + extra_ref[...]
    row = lax.broadcasted_iota(jnp.int32, (length, length), 0)
    column = lax.broadcasted_iota(jnp.int32, (length, length), 1)
    causal = row >= column
    cum = jnp.dot(causal.astype(F32), log_decay, precision=EXACT, preferred_element_type=F32)
    cum_ref[...] = cum
    cum_rows = cum.T
    lanes = head_lanes(heads)
    b = conv(b_ref, v_ref.shape[1], bk_ref, b_ext).astype(BF16)
    v = conv(v_ref, 0, vk_ref, v_ext)
    last = cum[length - 1 : length]
    weighted = v * expand(step, lanes)
    ending = (weighted * expand(jnp.exp(last - cum), lanes)).astype(BF16)
    weighted = weighted.astype(BF16)
    whole = expand(jnp.broadcast_to(last, (8, heads)), lanes)
    coarse = whole.astype(BF16)
    state_ref[STATE : STATE + 8] = coarse
    state_ref[STATE + 8 :] = (whole - coarse.astype(F32)).astype(BF16)
    for g in range(groups):
        span = slice(g * per_group * HEAD_DIM, (g + 1) * per_group * HEAD_DIM)
        state_ref[:STATE, span] = lax.dot_general(
            b[:, g * STATE : (g + 1) * STATE], ending[:, span], (((0,), (0,)), ((), ())),
            preferred_element_type=F32,
        ).astype(BF16)
    c = conv(c_ref, v_ref.shape[1] + b_ref.shape[1], ck_ref, c_ext).astype(BF16)
    readout_ref[...] = c
    direct = v * skip_ref[...]
    for g in range(groups):
        cols = slice(g * STATE, (g + 1) * STATE)
        scores = lax.dot_general(
            c[:, cols], b[:, cols], (((1,), (1,)), ((), ())), preferred_element_type=F32
        )
        for h in range(g * per_group, (g + 1) * per_group):
            span = slice(h * HEAD_DIM, (h + 1) * HEAD_DIM)
            logs = jnp.where(causal, cum[:, h : h + 1] - cum_rows[h : h + 1], -jnp.inf)
            mixed = (scores * jnp.exp(logs)).astype(BF16)
            y_ref[:, span] = direct[:, span] + jnp.dot(
                mixed, weighted[:, span], preferred_element_type=F32
            )


def joined_kernel(
    axis, states_ref, y_ref, readout_ref, cum_ref, gate_ref, gain_ref, out_w_ref, out_ref, heads_ref
):
    me = lax.axis_index(axis)
    count = states_ref.shape[0]
    length, heads = cum_ref.shape
    groups = readout_ref.shape[1] // STATE
    per_group = heads // groups
    width = heads * HEAD_DIM

    def hop(turn, carry):
        total, run = carry
        k = count - 1 - turn
        earlier = k < me
        block = states_ref[k].astype(F32)
        factor = jnp.where(earlier, jnp.exp(run), 0.0)
        total = total + factor * block[:STATE]
        span = block[STATE : STATE + 1] + block[STATE + 8 : STATE + 9]
        return total, run + jnp.where(earlier, span, 0.0)

    start = (jnp.zeros((STATE, width), F32), jnp.zeros((1, width), F32))
    incoming = lax.fori_loop(0, count, hop, start)[0].astype(BF16)
    lanes = head_lanes(heads)
    decayed = expand(jnp.exp(cum_ref[...]), lanes)
    parts = [
        jnp.dot(
            readout_ref[:, g * STATE : (g + 1) * STATE],
            incoming[:, g * per_group * HEAD_DIM : (g + 1) * per_group * HEAD_DIM],
            preferred_element_type=F32,
        )
        for g in range(groups)
    ]
    mixed = y_ref[...] + jnp.concatenate(parts, axis=1) * decayed
    mixed = mixed * silu(gate_ref[...].astype(F32))
    squares = lax.dot_general(
        mixed * mixed, lanes, (((1,), (1,)), ((), ())), precision=EXACT, preferred_element_type=F32
    )
    scale = expand(lax.rsqrt(squares / HEAD_DIM + EPSILON), lanes)
    heads_ref[...] = (mixed * scale * gain_ref[...]).astype(BF16)
    tile = 512
    for first in range(0, out_w_ref.shape[1], tile):
        out_ref[:, first : first + tile] = jnp.dot(
            heads_ref[...], out_w_ref[:, first : first + tile], preferred_element_type=F32
        ).astype(BF16)


VMEM = pl.BlockSpec(memory_space=pltpu.VMEM)


def mixer(
    output_gate, value, state, readout, pre, extra, vk, bk, ck, rates, skip, gain, out_weight
):
    length, heads = pre.shape
    width = value.shape[1]
    count = lax.axis_size("sp")
    tails = jnp.concatenate([x[length - 8 :] for x in (value, state, readout)], axis=1)
    rim = lax.ppermute(tails, "sp", [(k, k + 1) for k in range(count - 1)])
    shape = jax.ShapeDtypeStruct
    states, y, c, cum = pl.pallas_call(
        local_kernel,
        out_shape=(
            shape((STATE + 16, width), BF16),
            shape((length, width), F32),
            shape(readout.shape, BF16),
            shape((length, heads), F32),
        ),
        in_specs=[VMEM] * 11,
        out_specs=(VMEM,) * 4,
        scratch_shapes=[
            pltpu.VMEM((length + 8, width), F32),
            pltpu.VMEM((length + 8, state.shape[1]), F32),
            pltpu.VMEM((length + 8, readout.shape[1]), F32),
        ],
        compiler_params=pltpu.CompilerParams(vmem_limit_bytes=48 << 20),
        cost_estimate=pl.CostEstimate(flops=10**9, bytes_accessed=4 * 10**6, transcendentals=10**6),
    )(
        value, state, readout, rim, pre, extra, rates[None],
        jnp.repeat(skip, HEAD_DIM)[None], vk, bk, ck,
    )
    gathered = lax.all_gather(states, "sp")
    return pl.pallas_call(
        functools.partial(joined_kernel, "sp"),
        out_shape=shape((length, out_weight.shape[1]), BF16),
        in_specs=[VMEM] * 7,
        out_specs=VMEM,
        scratch_shapes=[pltpu.VMEM((length, width), BF16)],
        compiler_params=pltpu.CompilerParams(vmem_limit_bytes=56 << 20),
        cost_estimate=pl.CostEstimate(flops=10**9, bytes_accessed=9 * 10**6, transcendentals=10**6),
    )(gathered, y, c, cum, output_gate, gain[None], out_weight)


def shared_slices(gate, up, down):
    count, parts = lax.axis_size("sp"), lax.axis_size("tp")
    held = gate.shape[1]
    piece = held * parts // count
    s, t = lax.axis_index("sp"), lax.axis_index("tp")
    first = (s * piece) % held
    mine = jnp.concatenate(
        [lax.dynamic_slice_in_dim(w, first, piece, axis=1) for w in (gate, up, down)], axis=1
    )
    owner = [(k * piece) // held for k in range(count)]
    total = jnp.where(t == (s * piece) // held, mine, jnp.zeros_like(mine))
    for d in range(1, parts):
        pairs = [(k * parts + o, k * parts + (o + d) % parts) for k, o in enumerate(owner)]
        total = total + lax.ppermute(mine, ("sp", "tp"), pairs)
    return total[:, :piece], total[:, piece : 2 * piece], total[:, 2 * piece :]


def shards(
    residual,
    output_gate_projected,
    value_projected_input,
    state_projected_input,
    readout_projected_input,
    step_preactivation,
    position_decay_extra,
    value_conv_kernel,
    state_conv_kernel,
    readout_conv_kernel,
    head_log_decay_rates,
    head_direct_weight,
    head_norm_gain,
    mixer_output_weight,
    expert_norm_gain,
    routed_expert_index,
    routed_expert_weight,
    routed_gate_weight,
    routed_up_weight,
    routed_down_weight,
    common_gate_weight,
    common_up_weight,
    common_down_weight,
):
    shared_gate, shared_up, shared_down = shared_slices(
        common_gate_weight, common_up_weight, common_down_weight
    )
    partial_mix = mixer(
        output_gate_projected, value_projected_input, state_projected_input,
        readout_projected_input, step_preactivation, position_decay_extra, value_conv_kernel,
        state_conv_kernel, readout_conv_kernel, head_log_decay_rates, head_direct_weight,
        head_norm_gain, mixer_output_weight,
    )
    count = lax.axis_size("sp")
    local_experts = routed_gate_weight.shape[0]
    experts_all = local_experts * count
    row_count, features = residual.shape
    chosen = jnp.arange(experts_all, dtype=jnp.int32) == routed_expert_index[:, :, None]
    combine = jnp.sum(jnp.where(chosen, routed_expert_weight[:, :, None], 0.0), axis=1)
    combine_high = combine.astype(BF16)
    combine_low = (combine - combine_high.astype(F32)).astype(BF16)
    extra_lanes = -(-2 * experts_all // 128) * 128 - 2 * experts_all

    mix_sum = lax.psum_scatter(partial_mix, "tp", scatter_dimension=0, tiled=True).astype(F32)
    stream = (residual.astype(F32) + mix_sum).astype(BF16)
    stream_wide = stream.astype(F32)
    normed_rows = (
        stream_wide
        * lax.rsqrt(jnp.mean(stream_wide * stream_wide, axis=-1, keepdims=True) + EPSILON)
        * expert_norm_gain
    ).astype(BF16)
    packed = jnp.concatenate(
        [normed_rows, combine_high, combine_low, jnp.zeros((row_count, extra_lanes), BF16)], axis=1
    )
    gathered = lax.all_gather(packed, "sp", axis=0, tiled=True)
    rows = gathered[:, :features]
    marks = gathered[:, features:].astype(F32)
    weights = marks[:, :experts_all] + marks[:, experts_all : 2 * experts_all]
    first = lax.axis_index("sp") * local_experts
    dot = functools.partial(jnp.dot, preferred_element_type=F32)
    hidden = (jax.nn.silu(dot(rows, shared_gate)) * dot(rows, shared_up)).astype(BF16)
    result = lax.dot_general(
        hidden, shared_down, (((1,), (1,)), ((), ())), preferred_element_type=F32
    )
    for e in range(local_experts):
        weight = lax.dynamic_slice_in_dim(weights, first + e, 1, axis=1)
        hidden = (
            jax.nn.silu(dot(rows, routed_gate_weight[e])) * dot(rows, routed_up_weight[e])
        ).astype(BF16)
        result = result + weight * dot(hidden, routed_down_weight[e])
    added = lax.psum_scatter(result.astype(BF16), "sp", scatter_dimension=0, tiled=True)
    return (stream_wide + added.astype(F32)).astype(BF16)


def solution(mesh):
    placed = (
        P(("sp", "tp"), None),
        P("sp", "tp"),
        P("sp", "tp"),
        P("sp", "tp"),
        P("sp", "tp"),
        P("sp", "tp"),
        P("sp", "tp"),
        P(None, "tp"),
        P(None, "tp"),
        P(None, "tp"),
        P("tp"),
        P("tp"),
        P("tp"),
        P("tp", None),
        P(),
        P(("sp", "tp"), None),
        P(("sp", "tp"), None),
        P("sp", None, None),
        P("sp", None, None),
        P("sp", None, None),
        P(None, "tp"),
        P(None, "tp"),
        P(None, "tp"),
    )
    return jax.shard_map(
        shards, mesh=mesh, in_specs=placed, out_specs=P(("sp", "tp"), None), check_vma=False
    )
```

```python
import functools

import jax
import jax.numpy as jnp
from jax import lax
from jax.experimental import pallas as pl
from jax.experimental.pallas import tpu as pltpu
from jax.sharding import PartitionSpec as P

HEAD_DIM = 64
STATE = 128
CONV = 4
EPSILON = 1e-06
EXACT = lax.Precision.HIGHEST
F32 = jnp.float32
BF16 = jnp.bfloat16


def head_lanes(heads):
    lane_head = lax.broadcasted_iota(jnp.int32, (heads, heads * HEAD_DIM), 1) // HEAD_DIM
    return (lane_head == lax.broadcasted_iota(jnp.int32, lane_head.shape, 0)).astype(F32)


def expand(per_head, lanes):
    return jnp.dot(per_head, lanes, precision=EXACT, preferred_element_type=F32)


def silu(value):
    return value / (1.0 + jnp.exp(-value))


def local_kernel(
    v_ref, b_ref, c_ref, rim_ref, pre_ref, extra_ref, rates_ref, skip_ref, vk_ref, bk_ref, ck_ref,
    state_ref, y_ref, readout_ref, cum_ref, v_ext, b_ext, c_ext,
):
    length, heads = pre_ref.shape
    groups = b_ref.shape[1] // STATE
    per_group = heads // groups
    pad = rim_ref.shape[0]

    def conv(x_ref, first, k_ref, ext):
        width = x_ref.shape[1]
        ext[:pad] = rim_ref[:, first : first + width].astype(F32)
        ext[pad:] = x_ref[...].astype(F32)
        total = jnp.zeros((length, width), F32)
        for tap in range(CONV):
            start = pad - CONV + 1 + tap
            total += ext[start : start + length] * k_ref[tap : tap + 1].astype(F32)
        return silu(total)

    step = pre_ref[...]
    step = jnp.maximum(step, 0.0) + jnp.log1p(jnp.exp(-jnp.abs(step)))
    log_decay = -jnp.exp(rates_ref[...]) * step + extra_ref[...]
    row = lax.broadcasted_iota(jnp.int32, (length, length), 0)
    column = lax.broadcasted_iota(jnp.int32, (length, length), 1)
    causal = row >= column
    cum = jnp.dot(causal.astype(F32), log_decay, precision=EXACT, preferred_element_type=F32)
    cum_ref[...] = cum
    cum_rows = cum.T
    lanes = head_lanes(heads)
    b = conv(b_ref, v_ref.shape[1], bk_ref, b_ext).astype(BF16)
    v = conv(v_ref, 0, vk_ref, v_ext)
    last = cum[length - 1 : length]
    weighted = v * expand(step, lanes)
    ending = (weighted * expand(jnp.exp(last - cum), lanes)).astype(BF16)
    weighted = weighted.astype(BF16)
    whole = expand(jnp.broadcast_to(last, (8, heads)), lanes)
    coarse = whole.astype(BF16)
    state_ref[STATE : STATE + 8] = coarse
    state_ref[STATE + 8 :] = (whole - coarse.astype(F32)).astype(BF16)
    for g in range(groups):
        span = slice(g * per_group * HEAD_DIM, (g + 1) * per_group * HEAD_DIM)
        state_ref[:STATE, span] = lax.dot_general(
            b[:, g * STATE : (g + 1) * STATE], ending[:, span], (((0,), (0,)), ((), ())),
            preferred_element_type=F32,
        ).astype(BF16)
    c = conv(c_ref, v_ref.shape[1] + b_ref.shape[1], ck_ref, c_ext).astype(BF16)
    readout_ref[...] = c
    direct = v * skip_ref[...]
    for g in range(groups):
        cols = slice(g * STATE, (g + 1) * STATE)
        scores = lax.dot_general(
            c[:, cols], b[:, cols], (((1,), (1,)), ((), ())), preferred_element_type=F32
        )
        for h in range(g * per_group, (g + 1) * per_group):
            span = slice(h * HEAD_DIM, (h + 1) * HEAD_DIM)
            logs = jnp.where(causal, cum[:, h : h + 1] - cum_rows[h : h + 1], -jnp.inf)
            mixed = (scores * jnp.exp(logs)).astype(BF16)
            y_ref[:, span] = direct[:, span] + jnp.dot(
                mixed, weighted[:, span], preferred_element_type=F32
            )


def joined_kernel(
    axis, states_ref, y_ref, readout_ref, cum_ref, gate_ref, gain_ref, out_w_ref, out_ref, heads_ref
):
    me = lax.axis_index(axis)
    count = states_ref.shape[0]
    length, heads = cum_ref.shape
    groups = readout_ref.shape[1] // STATE
    per_group = heads // groups
    width = heads * HEAD_DIM

    def hop(turn, carry):
        total, run = carry
        k = count - 1 - turn
        earlier = k < me
        block = states_ref[k].astype(F32)
        factor = jnp.where(earlier, jnp.exp(run), 0.0)
        total = total + factor * block[:STATE]
        span = block[STATE : STATE + 1] + block[STATE + 8 : STATE + 9]
        return total, run + jnp.where(earlier, span, 0.0)

    start = (jnp.zeros((STATE, width), F32), jnp.zeros((1, width), F32))
    incoming = lax.fori_loop(0, count, hop, start)[0].astype(BF16)
    lanes = head_lanes(heads)
    decayed = expand(jnp.exp(cum_ref[...]), lanes)
    parts = [
        jnp.dot(
            readout_ref[:, g * STATE : (g + 1) * STATE],
            incoming[:, g * per_group * HEAD_DIM : (g + 1) * per_group * HEAD_DIM],
            preferred_element_type=F32,
        )
        for g in range(groups)
    ]
    mixed = y_ref[...] + jnp.concatenate(parts, axis=1) * decayed
    mixed = mixed * silu(gate_ref[...].astype(F32))
    squares = lax.dot_general(
        mixed * mixed, lanes, (((1,), (1,)), ((), ())), precision=EXACT, preferred_element_type=F32
    )
    scale = expand(lax.rsqrt(squares / HEAD_DIM + EPSILON), lanes)
    heads_ref[...] = (mixed * scale * gain_ref[...]).astype(BF16)
    tile = 512
    for first in range(0, out_w_ref.shape[1], tile):
        out_ref[:, first : first + tile] = jnp.dot(
            heads_ref[...], out_w_ref[:, first : first + tile], preferred_element_type=F32
        ).astype(BF16)


VMEM = pl.BlockSpec(memory_space=pltpu.VMEM)


MESH = pl.DeviceIdType.MESH
CUTS = 2


def greet(peers):
    barrier = pltpu.get_barrier_semaphore()
    for here, peer, axis in peers:
        @pl.when(here)
        def _():
            pl.semaphore_signal(barrier, inc=1, device_id={axis: peer}, device_id_type=MESH)
    pl.semaphore_wait(barrier, sum(jnp.where(here, 1, 0) for here, _, _ in peers))


def gather_kernel(spread, lines, *refs):
    if spread is None:
        x_ref, out_ref, sent, landed = refs
    else:
        x_ref, mine_ref, out_ref, slices_ref, sent, landed, spread_sent, spread_landed = refs
    me = lax.axis_index("sp")
    z, y = me // 2, me % 2
    half = x_ref.shape[0] // CUTS
    always = me >= 0
    peers = [
        (always, me + 1 - 2 * y, "sp"), (z > 0, me - 2, "sp"), (z < lines - 1, me + 2, "sp")
    ]
    if spread is not None:
        piece, held, parts = spread
        t = lax.axis_index("tp")
        owner = (me * piece) // held
        peers += [(always, (t + d) % parts, "tp") for d in range(1, parts)]
    greet(peers)

    def send(block, cut, way, peer, first):
        rows = pl.ds(cut * half, half)
        return pltpu.make_async_remote_copy(
            src_ref=x_ref.at[rows] if first else out_ref.at[block, rows],
            dst_ref=out_ref.at[block, rows],
            send_sem=sent.at[way, block, cut],
            recv_sem=landed.at[block, cut],
            device_id={"sp": peer},
            device_id_type=MESH,
        )

    for cut in range(CUTS):
        for way, (here, peer, _) in enumerate(peers[:3]):
            @pl.when(here)
            def _():
                send(me, cut, way, peer, True).start()
    if spread is not None:
        def share(d):
            return pltpu.make_async_remote_copy(
                src_ref=mine_ref, dst_ref=slices_ref, send_sem=spread_sent.at[d - 1],
                recv_sem=spread_landed.at[0], device_id={"tp": (t + d) % parts},
                device_id_type=MESH,
            )

        @pl.when(t == owner)
        def _():
            for d in range(1, parts):
                share(d).start()
            slices_ref[...] = mine_ref[...]

    out_ref[me] = x_ref[...]
    for turn in range(1, lines):
        for cut in range(CUTS):
            for step, onward in ((-1, 2), (1, 1)):
                far = z + step * turn
                block = far * 2 + y

                @pl.when((far >= 0) & (far < lines))
                def _():
                    send(block, cut, 0, peers[0][1], False).wait_recv()
                    send(block, cut, 0, peers[0][1], False).start()

                    @pl.when(peers[onward][0])
                    def _():
                        send(block, cut, onward, peers[onward][1], False).start()

    for line in range(lines):
        for cut in range(CUTS):
            send(line * 2 + 1 - y, cut, 0, peers[0][1], False).wait_recv()
    for cut in range(CUTS):
        for line in range(lines):
            send(line * 2 + y, cut, 0, peers[0][1], False).wait_send()

            @pl.when((line <= z) & peers[2][0])
            def _():
                send(line * 2 + y, cut, 2, peers[2][1], False).wait_send()

            @pl.when((line >= z) & peers[1][0])
            def _():
                send(line * 2 + y, cut, 1, peers[1][1], False).wait_send()

    if spread is not None:
        @pl.when(t == owner)
        def _():
            for d in range(1, parts):
                share(d).wait_send()

        @pl.when(t != owner)
        def _():
            share(1).wait_recv()


def gather_sp(x, number, mine=None, held=0):
    count, parts = lax.axis_size("sp"), lax.axis_size("tp")
    shape = jax.ShapeDtypeStruct
    lands = [shape((count, *x.shape), x.dtype)]
    sems = [pltpu.SemaphoreType.DMA((3, count, CUTS)), pltpu.SemaphoreType.DMA((count, CUTS))]
    operands, spread = [x], None
    if mine is not None:
        spread = (mine.shape[1] // 3, held, parts)
        operands.append(mine)
        lands.append(shape(mine.shape, mine.dtype))
        sems += [pltpu.SemaphoreType.DMA((parts - 1,)), pltpu.SemaphoreType.DMA((1,))]
    return pl.pallas_call(
        functools.partial(gather_kernel, spread, count // 2),
        out_shape=tuple(lands),
        in_specs=[VMEM] * len(operands),
        out_specs=(VMEM,) * len(lands),
        scratch_shapes=sems,
        compiler_params=pltpu.CompilerParams(
            collective_id=number, has_side_effects=True, vmem_limit_bytes=24 << 20
        ),
    )(*operands)


def reduce_sp_kernel(lines, x_ref, out_ref, across, along, staged, sent, landed, z_sent, z_landed):
    me = lax.axis_index("sp")
    z, y = me // 2, me % 2
    other = me + 1 - 2 * y
    half = out_ref.shape[0] // CUTS
    greet([(me >= 0, other, "sp"), (z > 0, me - 2, "sp"), (z < lines - 1, me + 2, "sp")])

    def cross(line, cut):
        rows = pl.ds(cut * half, half)
        return pltpu.make_async_remote_copy(
            src_ref=x_ref.at[line * 2 + 1 - y, rows], dst_ref=across.at[line, rows],
            send_sem=sent.at[line, cut], recv_sem=landed.at[line, cut],
            device_id={"sp": other}, device_id_type=MESH,
        )

    def forward(line, slot, cut, step):
        rows = pl.ds(cut * half, half)
        return pltpu.make_async_remote_copy(
            src_ref=staged.at[line, rows], dst_ref=along.at[slot, rows],
            send_sem=z_sent.at[line, cut], recv_sem=z_landed.at[slot, cut],
            device_id={"sp": me + 2 * step}, device_id_type=MESH,
        )

    for turn in reversed(range(lines)):
        for cut in range(CUTS):
            for step in (-1, 1) if turn else (1,):
                line = z + step * turn

                @pl.when((line >= 0) & (line < lines))
                def _():
                    cross(line, cut).start()

    def met(line, cut):
        rows = pl.ds(cut * half, half)
        cross(line, cut).wait_recv()
        return x_ref[line * 2 + y, rows].astype(F32) + across[line, rows].astype(F32)

    for turn in reversed(range(1, lines)):
        for cut in range(CUTS):
            rows = pl.ds(cut * half, half)
            for step in (-1, 1):
                line = z + step * turn
                behind = z - step
                inside = (line >= 0) & (line < lines)
                fed = (behind >= 0) & (behind < lines)
                slot = jnp.where((turn == 1) & (step < 0), lines, line)

                @pl.when(inside & fed)
                def _():
                    value = met(line, cut)
                    forward(line, line, cut, step).wait_recv()
                    staged[line, rows] = (value + along[line, rows].astype(F32)).astype(BF16)

                @pl.when(inside & jnp.logical_not(fed))
                def _():
                    staged[line, rows] = met(line, cut).astype(BF16)

                @pl.when(inside)
                def _():
                    forward(line, slot, cut, step).start()

    for cut in range(CUTS):
        rows = pl.ds(cut * half, half)
        staged[z, rows] = met(z, cut).astype(BF16)

        @pl.when(z > 0)
        def _():
            forward(z, z, cut, 1).wait_recv()
            staged[z, rows] = (staged[z, rows].astype(F32) + along[z, rows].astype(F32)).astype(BF16)

        @pl.when(z < lines - 1)
        def _():
            forward(z, lines, cut, -1).wait_recv()
            staged[z, rows] = (
                staged[z, rows].astype(F32) + along[lines, rows].astype(F32)
            ).astype(BF16)

        out_ref[rows] = staged[z, rows]
        for line in range(lines):
            cross(line, cut).wait_send()

            @pl.when(line != z)
            def _():
                forward(line, line, cut, 0).wait_send()


def reduce_sp(x, number):
    count = x.shape[0]
    lines = count // 2
    block = x.shape[1:]
    return pl.pallas_call(
        functools.partial(reduce_sp_kernel, lines),
        out_shape=jax.ShapeDtypeStruct(block, x.dtype),
        in_specs=[VMEM],
        out_specs=VMEM,
        scratch_shapes=[
            pltpu.VMEM((lines, *block), x.dtype),
            pltpu.VMEM((lines + 1, *block), x.dtype),
            pltpu.VMEM((lines, *block), x.dtype),
        ]
        + [
            pltpu.SemaphoreType.DMA((lines + extra, CUTS)) for extra in (0, 0, 0, 1)
        ],
        compiler_params=pltpu.CompilerParams(
            collective_id=number, has_side_effects=True, vmem_limit_bytes=24 << 20
        ),
    )(x)


def reduce_tp_kernel(x_ref, out_ref, near, staged, far, near_sent, near_landed, far_sent, far_landed):
    t = lax.axis_index("tp")
    a, b = t // 2, t % 2
    partner, opposite = a * 2 + 1 - b, (1 - a) * 2 + b
    always = t >= 0
    greet([(always, partner, "tp"), (always, opposite, "tp")])

    def swap(row):
        return pltpu.make_async_remote_copy(
            src_ref=x_ref.at[row * 2 + 1 - b], dst_ref=near.at[row],
            send_sem=near_sent.at[row], recv_sem=near_landed.at[row],
            device_id={"tp": partner}, device_id_type=MESH,
        )

    half = out_ref.shape[0] // CUTS

    def pass_on(cut):
        rows = pl.ds(cut * half, half)
        return pltpu.make_async_remote_copy(
            src_ref=staged.at[rows], dst_ref=far.at[rows],
            send_sem=far_sent.at[cut], recv_sem=far_landed.at[cut],
            device_id={"tp": opposite}, device_id_type=MESH,
        )

    swap(1 - a).start()
    swap(a).start()
    swap(1 - a).wait_recv()
    for cut in range(CUTS):
        rows = pl.ds(cut * half, half)
        staged[rows] = (
            x_ref[opposite, rows].astype(F32) + near[1 - a, rows].astype(F32)
        ).astype(BF16)
        pass_on(cut).start()
    swap(a).wait_recv()
    out_ref[...] = x_ref[t].astype(F32) + near[a].astype(F32)
    for cut in range(CUTS):
        rows = pl.ds(cut * half, half)
        pass_on(cut).wait_recv()
        out_ref[rows] += far[rows].astype(F32)
        pass_on(cut).wait_send()
    swap(0).wait_send()
    swap(1).wait_send()


def reduce_tp(x, number):
    parts, block = x.shape[0], x.shape[1:]
    return pl.pallas_call(
        reduce_tp_kernel,
        out_shape=jax.ShapeDtypeStruct(block, F32),
        in_specs=[VMEM],
        out_specs=VMEM,
        scratch_shapes=[
            pltpu.VMEM((parts // 2, *block), x.dtype),
            pltpu.VMEM(block, x.dtype),
            pltpu.VMEM(block, x.dtype),
        ]
        + [pltpu.SemaphoreType.DMA((2,))] * 2 + [pltpu.SemaphoreType.DMA((CUTS,))] * 2,
        compiler_params=pltpu.CompilerParams(
            collective_id=number, has_side_effects=True, vmem_limit_bytes=16 << 20
        ),
    )(x)


def small_mesh():
    return lax.axis_size("sp") in (4, 8) and lax.axis_size("tp") == 4


def mixer(
    output_gate, value, state, readout, pre, extra, vk, bk, ck, rates, skip, gain, out_weight,
    common,
):
    length, heads = pre.shape
    width = value.shape[1]
    count = lax.axis_size("sp")
    tails = jnp.concatenate([x[length - 8 :] for x in (value, state, readout)], axis=1)
    rim = lax.ppermute(tails, "sp", [(k, k + 1) for k in range(count - 1)])
    shape = jax.ShapeDtypeStruct
    states, y, c, cum = pl.pallas_call(
        local_kernel,
        out_shape=(
            shape((STATE + 16, width), BF16),
            shape((length, width), F32),
            shape(readout.shape, BF16),
            shape((length, heads), F32),
        ),
        in_specs=[VMEM] * 11,
        out_specs=(VMEM,) * 4,
        scratch_shapes=[
            pltpu.VMEM((length + 8, width), F32),
            pltpu.VMEM((length + 8, state.shape[1]), F32),
            pltpu.VMEM((length + 8, readout.shape[1]), F32),
        ],
        compiler_params=pltpu.CompilerParams(vmem_limit_bytes=48 << 20),
        cost_estimate=pl.CostEstimate(flops=10**9, bytes_accessed=4 * 10**6, transcendentals=10**6),
    )(
        value, state, readout, rim, pre, extra, rates[None],
        jnp.repeat(skip, HEAD_DIM)[None], vk, bk, ck,
    )
    if small_mesh():
        gathered, slices = gather_sp(states, 1, own_slices(*common), common[0].shape[1])
    else:
        gathered = lax.all_gather(states, "sp")
        slices = permuted_slices(*common)
    partial = pl.pallas_call(
        functools.partial(joined_kernel, "sp"),
        out_shape=shape((length, out_weight.shape[1]), BF16),
        in_specs=[VMEM] * 7,
        out_specs=VMEM,
        scratch_shapes=[pltpu.VMEM((length, width), BF16)],
        compiler_params=pltpu.CompilerParams(vmem_limit_bytes=56 << 20),
        cost_estimate=pl.CostEstimate(flops=10**9, bytes_accessed=9 * 10**6, transcendentals=10**6),
    )(gathered, y, c, cum, output_gate, gain[None], out_weight)
    return partial, slices


def own_slices(gate, up, down):
    held = gate.shape[1]
    piece = held * lax.axis_size("tp") // lax.axis_size("sp")
    first = (lax.axis_index("sp") * piece) % held
    return jnp.concatenate(
        [lax.dynamic_slice_in_dim(w, first, piece, axis=1) for w in (gate, up, down)], axis=1
    )


def permuted_slices(gate, up, down):
    count, parts = lax.axis_size("sp"), lax.axis_size("tp")
    held = gate.shape[1]
    mine = own_slices(gate, up, down)
    piece = mine.shape[1] // 3
    owner = [(k * piece) // held for k in range(count)]
    here = lax.axis_index("tp") == (lax.axis_index("sp") * piece) // held
    total = jnp.where(here, mine, jnp.zeros_like(mine))
    for d in range(1, parts):
        pairs = [(k * parts + o, k * parts + (o + d) % parts) for k, o in enumerate(owner)]
        total = total + lax.ppermute(mine, ("sp", "tp"), pairs)
    return total


def shards(
    residual,
    output_gate_projected,
    value_projected_input,
    state_projected_input,
    readout_projected_input,
    step_preactivation,
    position_decay_extra,
    value_conv_kernel,
    state_conv_kernel,
    readout_conv_kernel,
    head_log_decay_rates,
    head_direct_weight,
    head_norm_gain,
    mixer_output_weight,
    expert_norm_gain,
    routed_expert_index,
    routed_expert_weight,
    routed_gate_weight,
    routed_up_weight,
    routed_down_weight,
    common_gate_weight,
    common_up_weight,
    common_down_weight,
):
    partial_mix, slices = mixer(
        output_gate_projected, value_projected_input, state_projected_input,
        readout_projected_input, step_preactivation, position_decay_extra, value_conv_kernel,
        state_conv_kernel, readout_conv_kernel, head_log_decay_rates, head_direct_weight,
        head_norm_gain, mixer_output_weight,
        (common_gate_weight, common_up_weight, common_down_weight),
    )
    piece = slices.shape[1] // 3
    shared_gate, shared_up, shared_down = (
        slices[:, k * piece : (k + 1) * piece] for k in range(3)
    )
    count = lax.axis_size("sp")
    local_experts = routed_gate_weight.shape[0]
    experts_all = local_experts * count
    row_count, features = residual.shape
    chosen = jnp.arange(experts_all, dtype=jnp.int32) == routed_expert_index[:, :, None]
    combine = jnp.sum(jnp.where(chosen, routed_expert_weight[:, :, None], 0.0), axis=1)
    combine_high = combine.astype(BF16)
    combine_low = (combine - combine_high.astype(F32)).astype(BF16)
    extra_lanes = -(-2 * experts_all // 128) * 128 - 2 * experts_all

    if small_mesh():
        mix_sum = reduce_tp(partial_mix.reshape(-1, row_count, features), 2)
    else:
        mix_sum = lax.psum_scatter(partial_mix, "tp", scatter_dimension=0, tiled=True).astype(F32)
    stream = (residual.astype(F32) + mix_sum).astype(BF16)
    stream_wide = stream.astype(F32)
    normed_rows = (
        stream_wide
        * lax.rsqrt(jnp.mean(stream_wide * stream_wide, axis=-1, keepdims=True) + EPSILON)
        * expert_norm_gain
    ).astype(BF16)
    packed = jnp.concatenate(
        [normed_rows, combine_high, combine_low, jnp.zeros((row_count, extra_lanes), BF16)], axis=1
    )
    if small_mesh():
        gathered = gather_sp(packed, 3)[0].reshape(-1, packed.shape[1])
    else:
        gathered = lax.all_gather(packed, "sp", axis=0, tiled=True)
    rows = gathered[:, :features]
    marks = gathered[:, features:].astype(F32)
    weights = marks[:, :experts_all] + marks[:, experts_all : 2 * experts_all]
    first = lax.axis_index("sp") * local_experts
    dot = functools.partial(jnp.dot, preferred_element_type=F32)
    hidden = (jax.nn.silu(dot(rows, shared_gate)) * dot(rows, shared_up)).astype(BF16)
    result = lax.dot_general(
        hidden, shared_down, (((1,), (1,)), ((), ())), preferred_element_type=F32
    )
    for e in range(local_experts):
        weight = lax.dynamic_slice_in_dim(weights, first + e, 1, axis=1)
        hidden = (
            jax.nn.silu(dot(rows, routed_gate_weight[e])) * dot(rows, routed_up_weight[e])
        ).astype(BF16)
        result = result + weight * dot(hidden, routed_down_weight[e])
    result = result.astype(BF16)
    if small_mesh():
        added = reduce_sp(result.reshape(count, row_count, features), 4)
    else:
        added = lax.psum_scatter(result, "sp", scatter_dimension=0, tiled=True)
    return (stream_wide + added.astype(F32)).astype(BF16)


def solution(mesh):
    placed = (
        P(("sp", "tp"), None),
        P("sp", "tp"),
        P("sp", "tp"),
        P("sp", "tp"),
        P("sp", "tp"),
        P("sp", "tp"),
        P("sp", "tp"),
        P(None, "tp"),
        P(None, "tp"),
        P(None, "tp"),
        P("tp"),
        P("tp"),
        P("tp"),
        P("tp", None),
        P(),
        P(("sp", "tp"), None),
        P(("sp", "tp"), None),
        P("sp", None, None),
        P("sp", None, None),
        P("sp", None, None),
        P(None, "tp"),
        P(None, "tp"),
        P(None, "tp"),
    )
    return jax.shard_map(
        shards, mesh=mesh, in_specs=placed, out_specs=P(("sp", "tp"), None), check_vma=False
    )
```

```python
import functools

import jax
import jax.numpy as jnp
from jax import lax
from jax.experimental import pallas as pl
from jax.experimental.pallas import tpu as pltpu
from jax.sharding import PartitionSpec as P

HEAD_DIM = 64
STATE = 128
CONV = 4
EPSILON = 1e-06
EXACT = lax.Precision.HIGHEST
F32 = jnp.float32
BF16 = jnp.bfloat16


def head_lanes(heads):
    lane_head = lax.broadcasted_iota(jnp.int32, (heads, heads * HEAD_DIM), 1) // HEAD_DIM
    return (lane_head == lax.broadcasted_iota(jnp.int32, lane_head.shape, 0)).astype(F32)


def expand(per_head, lanes):
    return jnp.dot(per_head, lanes, precision=EXACT, preferred_element_type=F32)


def silu(value):
    return value / (1.0 + jnp.exp(-value))


def local_kernel(
    v_ref, b_ref, c_ref, rim_ref, pre_ref, extra_ref, rates_ref, skip_ref, vk_ref, bk_ref, ck_ref,
    state_ref, y_ref, readout_ref, cum_ref, v_ext, b_ext, c_ext,
):
    length, heads = pre_ref.shape
    groups = b_ref.shape[1] // STATE
    per_group = heads // groups
    pad = rim_ref.shape[0]

    def conv(x_ref, first, k_ref, ext):
        width = x_ref.shape[1]
        ext[:pad] = rim_ref[:, first : first + width].astype(F32)
        ext[pad:] = x_ref[...].astype(F32)
        total = jnp.zeros((length, width), F32)
        for tap in range(CONV):
            start = pad - CONV + 1 + tap
            total += ext[start : start + length] * k_ref[tap : tap + 1].astype(F32)
        return silu(total)

    step = pre_ref[...]
    step = jnp.maximum(step, 0.0) + jnp.log1p(jnp.exp(-jnp.abs(step)))
    log_decay = -jnp.exp(rates_ref[...]) * step + extra_ref[...]
    row = lax.broadcasted_iota(jnp.int32, (length, length), 0)
    column = lax.broadcasted_iota(jnp.int32, (length, length), 1)
    causal = row >= column
    cum = jnp.dot(causal.astype(F32), log_decay, precision=EXACT, preferred_element_type=F32)
    cum_ref[...] = cum
    cum_rows = cum.T
    lanes = head_lanes(heads)
    b = conv(b_ref, v_ref.shape[1], bk_ref, b_ext).astype(BF16)
    v = conv(v_ref, 0, vk_ref, v_ext)
    last = cum[length - 1 : length]
    weighted = v * expand(step, lanes)
    ending = (weighted * expand(jnp.exp(last - cum), lanes)).astype(BF16)
    weighted = weighted.astype(BF16)
    whole = expand(jnp.broadcast_to(last, (8, heads)), lanes)
    coarse = whole.astype(BF16)
    state_ref[STATE : STATE + 8] = coarse
    state_ref[STATE + 8 :] = (whole - coarse.astype(F32)).astype(BF16)
    for g in range(groups):
        span = slice(g * per_group * HEAD_DIM, (g + 1) * per_group * HEAD_DIM)
        state_ref[:STATE, span] = lax.dot_general(
            b[:, g * STATE : (g + 1) * STATE], ending[:, span], (((0,), (0,)), ((), ())),
            preferred_element_type=F32,
        ).astype(BF16)
    c = conv(c_ref, v_ref.shape[1] + b_ref.shape[1], ck_ref, c_ext).astype(BF16)
    readout_ref[...] = c
    direct = v * skip_ref[...]
    for g in range(groups):
        cols = slice(g * STATE, (g + 1) * STATE)
        scores = lax.dot_general(
            c[:, cols], b[:, cols], (((1,), (1,)), ((), ())), preferred_element_type=F32
        )
        for h in range(g * per_group, (g + 1) * per_group):
            span = slice(h * HEAD_DIM, (h + 1) * HEAD_DIM)
            logs = jnp.where(causal, cum[:, h : h + 1] - cum_rows[h : h + 1], -jnp.inf)
            mixed = (scores * jnp.exp(logs)).astype(BF16)
            y_ref[:, span] = direct[:, span] + jnp.dot(
                mixed, weighted[:, span], preferred_element_type=F32
            )


def joined_kernel(
    axis, states_ref, y_ref, readout_ref, cum_ref, gate_ref, gain_ref, out_w_ref, out_ref, heads_ref
):
    me = lax.axis_index(axis)
    count = states_ref.shape[0]
    length, heads = cum_ref.shape
    groups = readout_ref.shape[1] // STATE
    per_group = heads // groups
    width = heads * HEAD_DIM

    def hop(turn, carry):
        total, run = carry
        k = count - 1 - turn
        earlier = k < me
        block = states_ref[k].astype(F32)
        factor = jnp.where(earlier, jnp.exp(run), 0.0)
        total = total + factor * block[:STATE]
        span = block[STATE : STATE + 1] + block[STATE + 8 : STATE + 9]
        return total, run + jnp.where(earlier, span, 0.0)

    start = (jnp.zeros((STATE, width), F32), jnp.zeros((1, width), F32))
    incoming = lax.fori_loop(0, count, hop, start)[0].astype(BF16)
    lanes = head_lanes(heads)
    decayed = expand(jnp.exp(cum_ref[...]), lanes)
    parts = [
        jnp.dot(
            readout_ref[:, g * STATE : (g + 1) * STATE],
            incoming[:, g * per_group * HEAD_DIM : (g + 1) * per_group * HEAD_DIM],
            preferred_element_type=F32,
        )
        for g in range(groups)
    ]
    mixed = y_ref[...] + jnp.concatenate(parts, axis=1) * decayed
    mixed = mixed * silu(gate_ref[...].astype(F32))
    squares = lax.dot_general(
        mixed * mixed, lanes, (((1,), (1,)), ((), ())), precision=EXACT, preferred_element_type=F32
    )
    scale = expand(lax.rsqrt(squares / HEAD_DIM + EPSILON), lanes)
    heads_ref[...] = (mixed * scale * gain_ref[...]).astype(BF16)
    tile = 512
    for first in range(0, out_w_ref.shape[1], tile):
        out_ref[:, first : first + tile] = jnp.dot(
            heads_ref[...], out_w_ref[:, first : first + tile], preferred_element_type=F32
        ).astype(BF16)


VMEM = pl.BlockSpec(memory_space=pltpu.VMEM)


MESH = pl.DeviceIdType.MESH
CUTS = 4


def greet(peers):
    barrier = pltpu.get_barrier_semaphore()
    for here, peer, axis in peers:
        @pl.when(here)
        def _():
            pl.semaphore_signal(barrier, inc=1, device_id={axis: peer}, device_id_type=MESH)
    pl.semaphore_wait(barrier, sum(jnp.where(here, 1, 0) for here, _, _ in peers))


def cuts_of(rows):
    return next(cuts for cuts in (4, 3, 2, 1) if rows % (16 * cuts) == 0)


def gather_kernel(spread, lines, *refs):
    if spread is None:
        x_ref, out_ref, sent, landed = refs
    else:
        x_ref, mine_ref, out_ref, slices_ref, sent, landed, spread_sent, spread_landed = refs
    me = lax.axis_index("sp")
    z, y = me // 2, me % 2
    cuts = cuts_of(x_ref.shape[0])
    half = x_ref.shape[0] // cuts
    always = me >= 0
    peers = [
        (always, me + 1 - 2 * y, "sp"), (z > 0, me - 2, "sp"), (z < lines - 1, me + 2, "sp")
    ]
    if spread is not None:
        piece, held, parts = spread
        t = lax.axis_index("tp")
        owner = (me * piece) // held
        peers += [(always, (t + d) % parts, "tp") for d in range(1, parts)]
    greet(peers)

    def send(block, cut, way, peer, first):
        rows = pl.ds(cut * half, half)
        return pltpu.make_async_remote_copy(
            src_ref=x_ref.at[rows] if first else out_ref.at[block, rows],
            dst_ref=out_ref.at[block, rows],
            send_sem=sent.at[way, block, cut],
            recv_sem=landed.at[block, cut],
            device_id={"sp": peer},
            device_id_type=MESH,
        )

    for cut in range(cuts):
        for way, (here, peer, _) in enumerate(peers[:3]):
            @pl.when(here)
            def _():
                send(me, cut, way, peer, True).start()
    if spread is not None:
        def share(d):
            return pltpu.make_async_remote_copy(
                src_ref=mine_ref, dst_ref=slices_ref, send_sem=spread_sent.at[d - 1],
                recv_sem=spread_landed.at[0], device_id={"tp": (t + d) % parts},
                device_id_type=MESH,
            )

        @pl.when(t == owner)
        def _():
            for d in range(1, parts):
                share(d).start()
            slices_ref[...] = mine_ref[...]

    out_ref[me] = x_ref[...]
    for turn in range(1, lines):
        for cut in range(cuts):
            for step, onward in ((-1, 2), (1, 1)):
                far = z + step * turn
                block = far * 2 + y

                @pl.when((far >= 0) & (far < lines))
                def _():
                    send(block, cut, 0, peers[0][1], False).wait_recv()
                    send(block, cut, 0, peers[0][1], False).start()

                    @pl.when(peers[onward][0])
                    def _():
                        send(block, cut, onward, peers[onward][1], False).start()

    for line in range(lines):
        for cut in range(cuts):
            send(line * 2 + 1 - y, cut, 0, peers[0][1], False).wait_recv()
    for cut in range(cuts):
        for line in range(lines):
            send(line * 2 + y, cut, 0, peers[0][1], False).wait_send()

            @pl.when((line <= z) & peers[2][0])
            def _():
                send(line * 2 + y, cut, 2, peers[2][1], False).wait_send()

            @pl.when((line >= z) & peers[1][0])
            def _():
                send(line * 2 + y, cut, 1, peers[1][1], False).wait_send()

    if spread is not None:
        @pl.when(t == owner)
        def _():
            for d in range(1, parts):
                share(d).wait_send()

        @pl.when(t != owner)
        def _():
            share(1).wait_recv()


def gather_sp(x, number, mine=None, held=0):
    count, parts = lax.axis_size("sp"), lax.axis_size("tp")
    shape, cuts = jax.ShapeDtypeStruct, cuts_of(x.shape[0])
    lands = [shape((count, *x.shape), x.dtype)]
    sems = [pltpu.SemaphoreType.DMA((3, count, cuts)), pltpu.SemaphoreType.DMA((count, cuts))]
    operands, spread = [x], None
    if mine is not None:
        spread = (mine.shape[1] // 3, held, parts)
        operands.append(mine)
        lands.append(shape(mine.shape, mine.dtype))
        sems += [pltpu.SemaphoreType.DMA((parts - 1,)), pltpu.SemaphoreType.DMA((1,))]
    return pl.pallas_call(
        functools.partial(gather_kernel, spread, count // 2),
        out_shape=tuple(lands),
        in_specs=[VMEM] * len(operands),
        out_specs=(VMEM,) * len(lands),
        scratch_shapes=sems,
        compiler_params=pltpu.CompilerParams(
            collective_id=number, has_side_effects=True, vmem_limit_bytes=24 << 20
        ),
    )(*operands)


def reduce_sp_kernel(lines, x_ref, out_ref, across, along, staged, sent, landed, z_sent, z_landed):
    me = lax.axis_index("sp")
    z, y = me // 2, me % 2
    other = me + 1 - 2 * y
    half = out_ref.shape[0] // CUTS
    greet([(me >= 0, other, "sp"), (z > 0, me - 2, "sp"), (z < lines - 1, me + 2, "sp")])

    def cross(line, cut):
        rows = pl.ds(cut * half, half)
        return pltpu.make_async_remote_copy(
            src_ref=x_ref.at[line * 2 + 1 - y, rows], dst_ref=across.at[line, rows],
            send_sem=sent.at[line, cut], recv_sem=landed.at[line, cut],
            device_id={"sp": other}, device_id_type=MESH,
        )

    def forward(line, slot, cut, step):
        rows = pl.ds(cut * half, half)
        return pltpu.make_async_remote_copy(
            src_ref=staged.at[line, rows], dst_ref=along.at[slot, rows],
            send_sem=z_sent.at[line, cut], recv_sem=z_landed.at[slot, cut],
            device_id={"sp": me + 2 * step}, device_id_type=MESH,
        )

    for turn in reversed(range(lines)):
        for cut in range(CUTS):
            for step in (-1, 1) if turn else (1,):
                line = z + step * turn

                @pl.when((line >= 0) & (line < lines))
                def _():
                    cross(line, cut).start()

    def met(line, cut):
        rows = pl.ds(cut * half, half)
        cross(line, cut).wait_recv()
        return x_ref[line * 2 + y, rows].astype(F32) + across[line, rows].astype(F32)

    for turn in reversed(range(1, lines)):
        for cut in range(CUTS):
            rows = pl.ds(cut * half, half)
            for step in (-1, 1):
                line = z + step * turn
                behind = z - step
                inside = (line >= 0) & (line < lines)
                fed = (behind >= 0) & (behind < lines)
                slot = jnp.where((turn == 1) & (step < 0), lines, line)

                @pl.when(inside & fed)
                def _():
                    value = met(line, cut)
                    forward(line, line, cut, step).wait_recv()
                    staged[line, rows] = (value + along[line, rows].astype(F32)).astype(BF16)

                @pl.when(inside & jnp.logical_not(fed))
                def _():
                    staged[line, rows] = met(line, cut).astype(BF16)

                @pl.when(inside)
                def _():
                    forward(line, slot, cut, step).start()

    for cut in range(CUTS):
        rows = pl.ds(cut * half, half)
        staged[z, rows] = met(z, cut).astype(BF16)

        @pl.when(z > 0)
        def _():
            forward(z, z, cut, 1).wait_recv()
            staged[z, rows] = (staged[z, rows].astype(F32) + along[z, rows].astype(F32)).astype(BF16)

        @pl.when(z < lines - 1)
        def _():
            forward(z, lines, cut, -1).wait_recv()
            staged[z, rows] = (
                staged[z, rows].astype(F32) + along[lines, rows].astype(F32)
            ).astype(BF16)

        out_ref[rows] = staged[z, rows]
        for line in range(lines):
            cross(line, cut).wait_send()

            @pl.when(line != z)
            def _():
                forward(line, line, cut, 0).wait_send()


def reduce_sp(x, number):
    count = x.shape[0]
    lines = count // 2
    block = x.shape[1:]
    return pl.pallas_call(
        functools.partial(reduce_sp_kernel, lines),
        out_shape=jax.ShapeDtypeStruct(block, x.dtype),
        in_specs=[VMEM],
        out_specs=VMEM,
        scratch_shapes=[
            pltpu.VMEM((lines, *block), x.dtype),
            pltpu.VMEM((lines + 1, *block), x.dtype),
            pltpu.VMEM((lines, *block), x.dtype),
        ]
        + [
            pltpu.SemaphoreType.DMA((lines + extra, CUTS)) for extra in (0, 0, 0, 1)
        ],
        compiler_params=pltpu.CompilerParams(
            collective_id=number, has_side_effects=True, vmem_limit_bytes=24 << 20
        ),
    )(x)


def reduce_tp_kernel(x_ref, out_ref, near, staged, far, near_sent, near_landed, far_sent, far_landed):
    t = lax.axis_index("tp")
    a, b = t // 2, t % 2
    partner, opposite = a * 2 + 1 - b, (1 - a) * 2 + b
    always = t >= 0
    greet([(always, partner, "tp"), (always, opposite, "tp")])

    def swap(row):
        return pltpu.make_async_remote_copy(
            src_ref=x_ref.at[row * 2 + 1 - b], dst_ref=near.at[row],
            send_sem=near_sent.at[row], recv_sem=near_landed.at[row],
            device_id={"tp": partner}, device_id_type=MESH,
        )

    half = out_ref.shape[0] // CUTS

    def pass_on(cut):
        rows = pl.ds(cut * half, half)
        return pltpu.make_async_remote_copy(
            src_ref=staged.at[rows], dst_ref=far.at[rows],
            send_sem=far_sent.at[cut], recv_sem=far_landed.at[cut],
            device_id={"tp": opposite}, device_id_type=MESH,
        )

    swap(1 - a).start()
    swap(a).start()
    swap(1 - a).wait_recv()
    for cut in range(CUTS):
        rows = pl.ds(cut * half, half)
        staged[rows] = (
            x_ref[opposite, rows].astype(F32) + near[1 - a, rows].astype(F32)
        ).astype(BF16)
        pass_on(cut).start()
    swap(a).wait_recv()
    out_ref[...] = x_ref[t].astype(F32) + near[a].astype(F32)
    for cut in range(CUTS):
        rows = pl.ds(cut * half, half)
        pass_on(cut).wait_recv()
        out_ref[rows] += far[rows].astype(F32)
        pass_on(cut).wait_send()
    swap(0).wait_send()
    swap(1).wait_send()


def reduce_tp(x, number):
    parts, block = x.shape[0], x.shape[1:]
    return pl.pallas_call(
        reduce_tp_kernel,
        out_shape=jax.ShapeDtypeStruct(block, F32),
        in_specs=[VMEM],
        out_specs=VMEM,
        scratch_shapes=[
            pltpu.VMEM((parts // 2, *block), x.dtype),
            pltpu.VMEM(block, x.dtype),
            pltpu.VMEM(block, x.dtype),
        ]
        + [pltpu.SemaphoreType.DMA((2,))] * 2 + [pltpu.SemaphoreType.DMA((CUTS,))] * 2,
        compiler_params=pltpu.CompilerParams(
            collective_id=number, has_side_effects=True, vmem_limit_bytes=16 << 20
        ),
    )(x)


def small_mesh():
    return lax.axis_size("sp") in (4, 8) and lax.axis_size("tp") == 4


def expert_kernel(tile, experts_all, rows_ref, slices_ref, gate_ref, up_ref, down_ref, out_ref):
    local, features = gate_ref.shape[:2]
    piece = slices_ref.shape[1] // 3
    first = lax.axis_index("sp") * local
    dot = functools.partial(jnp.dot, preferred_element_type=F32)

    def chunk(number, _):
        at = pl.ds(pl.multiple_of(number * tile, tile), tile)
        rows = rows_ref[at, :features]
        marks = rows_ref[at, features:].astype(F32)
        lane = lax.broadcasted_iota(jnp.int32, marks.shape, 1)
        both = dot(rows, slices_ref[:, : 2 * piece])
        shared = (silu(both[:, :piece]) * both[:, piece:]).astype(BF16)
        hidden = []
        for e in range(local):
            named = (lane == first + e) | (lane == first + e + experts_all)
            weight = jnp.sum(jnp.where(named, marks, 0.0), axis=1, keepdims=True)
            opened = (silu(dot(rows, gate_ref[e])) * dot(rows, up_ref[e])).astype(BF16)
            hidden.append((opened, weight))
        wide = 512
        for begin in range(0, features, wide):
            cols = slice(begin, begin + wide)
            total = lax.dot_general(
                shared, slices_ref[cols, 2 * piece :], (((1,), (1,)), ((), ())),
                preferred_element_type=F32,
            )
            for e, (opened, weight) in enumerate(hidden):
                total += weight * dot(opened, down_ref[e, :, cols])
            out_ref[at, cols] = total.astype(BF16)
        return 0

    lax.fori_loop(0, rows_ref.shape[0] // tile, chunk, 0)


def experts(rows, slices, gate, up, down, experts_all):
    return pl.pallas_call(
        functools.partial(expert_kernel, 256, experts_all),
        out_shape=jax.ShapeDtypeStruct((rows.shape[0], gate.shape[1]), BF16),
        in_specs=[VMEM] * 5,
        out_specs=VMEM,
        compiler_params=pltpu.CompilerParams(vmem_limit_bytes=56 << 20),
        cost_estimate=pl.CostEstimate(
            flops=2 * 10**9, bytes_accessed=8 * 10**6, transcendentals=10**5
        ),
    )(rows, slices, gate, up, down)


def mixer(
    output_gate, value, state, readout, pre, extra, vk, bk, ck, rates, skip, gain, out_weight,
    common,
):
    length, heads = pre.shape
    width = value.shape[1]
    count = lax.axis_size("sp")
    tails = jnp.concatenate([x[length - 8 :] for x in (value, state, readout)], axis=1)
    rim = lax.ppermute(tails, "sp", [(k, k + 1) for k in range(count - 1)])
    shape = jax.ShapeDtypeStruct
    states, y, c, cum = pl.pallas_call(
        local_kernel,
        out_shape=(
            shape((STATE + 16, width), BF16),
            shape((length, width), F32),
            shape(readout.shape, BF16),
            shape((length, heads), F32),
        ),
        in_specs=[VMEM] * 11,
        out_specs=(VMEM,) * 4,
        scratch_shapes=[
            pltpu.VMEM((length + 8, width), F32),
            pltpu.VMEM((length + 8, state.shape[1]), F32),
            pltpu.VMEM((length + 8, readout.shape[1]), F32),
        ],
        compiler_params=pltpu.CompilerParams(vmem_limit_bytes=48 << 20),
        cost_estimate=pl.CostEstimate(flops=10**9, bytes_accessed=4 * 10**6, transcendentals=10**6),
    )(
        value, state, readout, rim, pre, extra, rates[None],
        jnp.repeat(skip, HEAD_DIM)[None], vk, bk, ck,
    )
    if small_mesh():
        gathered, slices = gather_sp(states, 1, own_slices(*common), common[0].shape[1])
    else:
        gathered = lax.all_gather(states, "sp")
        slices = permuted_slices(*common)
    partial = pl.pallas_call(
        functools.partial(joined_kernel, "sp"),
        out_shape=shape((length, out_weight.shape[1]), BF16),
        in_specs=[VMEM] * 7,
        out_specs=VMEM,
        scratch_shapes=[pltpu.VMEM((length, width), BF16)],
        compiler_params=pltpu.CompilerParams(vmem_limit_bytes=56 << 20),
        cost_estimate=pl.CostEstimate(flops=10**9, bytes_accessed=9 * 10**6, transcendentals=10**6),
    )(gathered, y, c, cum, output_gate, gain[None], out_weight)
    return partial, slices


def own_slices(gate, up, down):
    held = gate.shape[1]
    piece = held * lax.axis_size("tp") // lax.axis_size("sp")
    first = (lax.axis_index("sp") * piece) % held
    return jnp.concatenate(
        [lax.dynamic_slice_in_dim(w, first, piece, axis=1) for w in (gate, up, down)], axis=1
    )


def permuted_slices(gate, up, down):
    count, parts = lax.axis_size("sp"), lax.axis_size("tp")
    held = gate.shape[1]
    mine = own_slices(gate, up, down)
    piece = mine.shape[1] // 3
    owner = [(k * piece) // held for k in range(count)]
    here = lax.axis_index("tp") == (lax.axis_index("sp") * piece) // held
    total = jnp.where(here, mine, jnp.zeros_like(mine))
    for d in range(1, parts):
        pairs = [(k * parts + o, k * parts + (o + d) % parts) for k, o in enumerate(owner)]
        total = total + lax.ppermute(mine, ("sp", "tp"), pairs)
    return total


def shards(
    residual,
    output_gate_projected,
    value_projected_input,
    state_projected_input,
    readout_projected_input,
    step_preactivation,
    position_decay_extra,
    value_conv_kernel,
    state_conv_kernel,
    readout_conv_kernel,
    head_log_decay_rates,
    head_direct_weight,
    head_norm_gain,
    mixer_output_weight,
    expert_norm_gain,
    routed_expert_index,
    routed_expert_weight,
    routed_gate_weight,
    routed_up_weight,
    routed_down_weight,
    common_gate_weight,
    common_up_weight,
    common_down_weight,
):
    partial_mix, slices = mixer(
        output_gate_projected, value_projected_input, state_projected_input,
        readout_projected_input, step_preactivation, position_decay_extra, value_conv_kernel,
        state_conv_kernel, readout_conv_kernel, head_log_decay_rates, head_direct_weight,
        head_norm_gain, mixer_output_weight,
        (common_gate_weight, common_up_weight, common_down_weight),
    )
    count = lax.axis_size("sp")
    local_experts = routed_gate_weight.shape[0]
    experts_all = local_experts * count
    row_count, features = residual.shape
    chosen = jnp.arange(experts_all, dtype=jnp.int32) == routed_expert_index[:, :, None]
    combine = jnp.sum(jnp.where(chosen, routed_expert_weight[:, :, None], 0.0), axis=1)
    combine_high = combine.astype(BF16)
    combine_low = (combine - combine_high.astype(F32)).astype(BF16)
    extra_lanes = -(-2 * experts_all // 128) * 128 - 2 * experts_all

    if small_mesh():
        mix_sum = reduce_tp(partial_mix.reshape(-1, row_count, features), 2)
    else:
        mix_sum = lax.psum_scatter(partial_mix, "tp", scatter_dimension=0, tiled=True).astype(F32)
    stream = (residual.astype(F32) + mix_sum).astype(BF16)
    stream_wide = stream.astype(F32)
    normed_rows = (
        stream_wide
        * lax.rsqrt(jnp.mean(stream_wide * stream_wide, axis=-1, keepdims=True) + EPSILON)
        * expert_norm_gain
    ).astype(BF16)
    packed = jnp.concatenate(
        [normed_rows, combine_high, combine_low, jnp.zeros((row_count, extra_lanes), BF16)], axis=1
    )
    if small_mesh():
        gathered = gather_sp(packed, 3)[0].reshape(-1, packed.shape[1])
    else:
        gathered = lax.all_gather(packed, "sp", axis=0, tiled=True)
    result = experts(
        gathered, slices, routed_gate_weight, routed_up_weight, routed_down_weight, experts_all
    )
    if small_mesh():
        added = reduce_sp(result.reshape(count, row_count, features), 4)
    else:
        added = lax.psum_scatter(result, "sp", scatter_dimension=0, tiled=True)
    return (stream_wide + added.astype(F32)).astype(BF16)


def solution(mesh):
    placed = (
        P(("sp", "tp"), None),
        P("sp", "tp"),
        P("sp", "tp"),
        P("sp", "tp"),
        P("sp", "tp"),
        P("sp", "tp"),
        P("sp", "tp"),
        P(None, "tp"),
        P(None, "tp"),
        P(None, "tp"),
        P("tp"),
        P("tp"),
        P("tp"),
        P("tp", None),
        P(),
        P(("sp", "tp"), None),
        P(("sp", "tp"), None),
        P("sp", None, None),
        P("sp", None, None),
        P("sp", None, None),
        P(None, "tp"),
        P(None, "tp"),
        P(None, "tp"),
    )
    return jax.shard_map(
        shards, mesh=mesh, in_specs=placed, out_specs=P(("sp", "tp"), None), check_vma=False
    )
```
